256 devices in a mesh: rep: 2 (over z_hi), fs: 16 (over z_lo, y), tp: 8 (over x, core).
Axes of the slice: x: 4, y: 4, z: 8 (z_hi: 2, z_lo: 4; z = z_hi * 4 + z_lo), core: 2. Of those that a mesh axis runs over, the one named last changes fastest.
Arguments:
- inputs: bfloat16 [32768, 2048], P(('rep', 'fs', 'tp')), may hold values from -24 to 24
- cotangent: bfloat16 [32768, 2048], P(('rep', 'fs', 'tp')), may hold values from -24 to 24
- up_weight: bfloat16 [2048, 4096], P('fs', 'tp'), may hold values from -0.125 to 0.125
- down_weight: bfloat16 [4096, 2048], P('tp', 'fs'), may hold values from -0.09375 to 0.09375
Outputs:
- input_grad: bfloat16 [32768, 2048], P(('rep', 'fs', 'tp'))
- up_grad: float32 [2048, 4096], P('fs', 'tp')
- down_grad: float32 [4096, 2048], P('tp', 'fs')
The draws below stay inside these ranges and needn't reach their ends.
All inputs are finite; a program needn't handle non-finite values.
Results may differ from the reference program's by a relative error of at most 0.013.
Values may be sent and summed in bfloat16 or wider, within the bound.
No kernel may reach another device: no remote copies, remote signals or barrier semaphores. Data moves between devices by JAX's collectives and lax.ppermute only.
A program may use at most 128 MiB of HBM per device.

```python
import jax
import jax.numpy as jnp
from jax import lax

D = 2048
FF = 4096
TOKENS = 32768
N_TP = 8


def raised(array, stream_key, source, target, blocks, factor):
    owner, partner = [(jnp.arange(array.shape[dim]) // (array.shape[dim] // blocks)).reshape([-1 if axis == dim else 1 for axis in range(array.ndim)]) for dim in (source, target)]
    chosen = jax.random.permutation(stream_key, blocks)[partner]
    strong = (owner == chosen) | (owner == (partner + blocks // 2) % blocks)
    return jnp.where(strong, factor * array, array)


def shard_levels(key, shape, pieces, low, top_value):
    def one(axis_at, blocks):
        steps = jax.random.uniform(jax.random.fold_in(jax.random.fold_in(key, 6), axis_at), (blocks,), jnp.float32, low / len(pieces), top_value / len(pieces))
        return jnp.repeat(jnp.exp(steps), shape[axis_at] // blocks).reshape((-1,) + (1,) * (len(shape) - axis_at - 1))

    level = one(*pieces[0])
    for cut in pieces[1:]:
        level = level * one(*cut)
    return level


def gaussian(key, shape, scale, bound, cuts=(), held_as=jnp.bfloat16):
    level = shard_levels(key, shape, cuts, -0.22, 0.18) if cuts else 1.0
    drawn = jax.random.normal(key, shape, jnp.float32) * scale * level
    return jnp.minimum(jnp.maximum(drawn, -bound), bound).astype(held_as)


def noise_with(stream_key, dims, deviation, bound, pieces, heavy, held_as=jnp.bfloat16):
    entries = deviation * jax.random.normal(stream_key, dims, jnp.float32)
    if pieces:
        entries = entries * shard_levels(stream_key, dims, pieces, -0.22, 0.18)
    return jnp.clip(raised(entries, jax.random.fold_in(stream_key, 3), *heavy), -bound, bound).astype(held_as)


def setup_inputs(seed: int = 0) -> dict:
    key_list = jax.random.split(jax.random.key(seed), 5)
    inputs = noise_with(key_list[0], (TOKENS, D), 1.0, 24.0, ((0, 256),), (0, 1, 256, 6.0))
    cotangent = noise_with(key_list[1], (TOKENS, D), 1.0, 24.0, ((0, 256),), (0, 1, 256, 6.0))
    up_weight = gaussian(key_list[2], (D, FF), D ** -0.5, 0.125, ((0, 16), (1, 8)))
    down_weight = gaussian(key_list[3], (FF, D), FF ** -0.5, 0.09375, ((0, 8), (1, 16)))
    return dict(inputs=inputs, cotangent=cotangent, up_weight=up_weight, down_weight=down_weight)


def reference(inputs, cotangent, up_weight, down_weight):
    pre_active = jnp.dot(inputs, up_weight, preferred_element_type=jnp.float32)
    active = jnp.maximum(pre_active, 0.0)
    activation = (active * active).astype(jnp.bfloat16)
    activation_grad = jnp.dot(cotangent, down_weight.T, preferred_element_type=jnp.float32)
    pre_grad = (2.0 * active * activation_grad).astype(jnp.bfloat16)
    block_width = FF // N_TP

    def add_block(index, running):
        offset = (index * block_width).astype(jnp.int32)
        grad_cols = lax.dynamic_slice_in_dim(pre_grad, offset, block_width, 1)
        weight_cols = lax.dynamic_slice_in_dim(up_weight, offset, block_width, 1)
        partial_sum = jnp.dot(grad_cols, weight_cols.T, preferred_element_type=jnp.float32)
        rounded = lax.optimization_barrier(partial_sum.astype(jnp.bfloat16))
        return running + rounded.astype(jnp.float32)

    start_sum = jnp.zeros((inputs.shape[0], D), jnp.float32)
    input_grad = lax.fori_loop(jnp.int32(0), jnp.int32(N_TP), add_block, start_sum).astype(jnp.bfloat16)
    loss_scale = TOKENS ** -0.5
    up_grad = jnp.dot(inputs.T, pre_grad, preferred_element_type=jnp.float32) * loss_scale
    down_grad = jnp.dot(activation.T, cotangent, preferred_element_type=jnp.float32) * loss_scale
    return (input_grad, up_grad, down_grad)
```

```python
import functools
import math

import jax
import jax.numpy as jnp
from jax import lax
from jax.experimental import pallas as pl
from jax.experimental.pallas import tpu as pltpu
from jax.sharding import Mesh
from jax.sharding import PartitionSpec as P


ALL = ("rep", "z", "y", "x", "core")
RING = {"z": (("rep", "z"), 8), "y": ("y", 4), "x": ("x", 4)}
F32, BF16 = jnp.float32, jnp.bfloat16


def shift(v, axis, by):
    name, n = RING[axis]
    return lax.ppermute(v, name, [(i, (i + by) % n) for i in range(n)])


def swap(v, axis):
    return lax.ppermute(v, axis, [(0, 1), (1, 0)])


def gathered(v, axis):
    half = v.shape[0] // 2
    below, above = shift(v, axis, 1), shift(v, axis, -1)
    far = jnp.concatenate([shift(below[:half], axis, 1), shift(above[half:], axis, -1)], axis=0)
    return [v, above, far, below]


def scattered(g, axis):
    half = g[0].shape[0] // 2
    up = shift(g[2][:half], axis, 1)
    down = shift(g[2][half:], axis, -1)
    first = jnp.concatenate([add(g[1][:half], up), g[1][half:]], axis=0)
    third = jnp.concatenate([g[3][:half], add(g[3][half:], down)], axis=0)
    a, b = shift(first, axis, 1), shift(third, axis, -1)
    return g[0].astype(F32) + a.astype(F32) + b.astype(F32)


def add(a, b):
    return (a.astype(F32) + b.astype(F32)).astype(BF16)


def rotate(where, y_major, x):
    def kernel(at, x_ref, o_ref):
        for j in range(16):
            a, b = j // 4, j % 4
            ry, rz = (a, b) if y_major else (b, a)
            src = lax.rem(at[0] + rz, 4) * 4 + lax.rem(at[1] + ry, 4)
            o_ref[:, j * 128 : (j + 1) * 128] = x_ref[:, pl.ds(pl.multiple_of(src * 128, 128), 128)]

    return pl.pallas_call(
        kernel,
        out_shape=jax.ShapeDtypeStruct(x.shape, x.dtype),
        in_specs=[pl.BlockSpec(memory_space=pltpu.SMEM), pl.BlockSpec(memory_space=pltpu.VMEM)],
        out_specs=pl.BlockSpec(memory_space=pltpu.VMEM),
        cost_estimate=pl.CostEstimate(flops=4_000_000, bytes_accessed=2 * x.size * 2, transcendentals=0),
        name="rotate",
    )(where, x)


def unrotate(where, y_major, x):
    def kernel(at, x_ref, o_ref):
        for j in range(16):
            a, b = j // 4, j % 4
            ry, rz = (a, b) if y_major else (b, a)
            dst = lax.rem(at[0] + rz, 4) * 4 + lax.rem(at[1] + ry, 4)
            o_ref[:, pl.ds(pl.multiple_of(dst * 128, 128), 128)] = x_ref[:, j * 128 : (j + 1) * 128].astype(BF16)

    return pl.pallas_call(
        kernel,
        out_shape=jax.ShapeDtypeStruct(x.shape, BF16),
        in_specs=[pl.BlockSpec(memory_space=pltpu.SMEM), pl.BlockSpec(memory_space=pltpu.VMEM)],
        out_specs=pl.BlockSpec(memory_space=pltpu.VMEM),
        cost_estimate=pl.CostEstimate(flops=4_000_000, bytes_accessed=2 * x.size * 4, transcendentals=0),
        name="unrotate",
    )(where, x)


def weight(shard, first, second):
    slab = jnp.concatenate(gathered(shard, first), axis=0)
    whole = jnp.concatenate(gathered(slab, second), axis=0)
    return jnp.concatenate([whole, swap(whole, "core")], axis=1)


def grad(rows, cols, first, second, scale):
    def product(a, b, out):
        return lax.dot_general(a, b, (((0,), (0,)), ((), ())), preferred_element_type=F32).astype(out)

    other = swap(product(rows, cols[:, 512:], BF16), "core")
    own = []
    for j in range(4):
        part = product(rows[:, j * 512 : (j + 1) * 512], cols[:, :512], F32)
        part = part + other[j * 512 : (j + 1) * 512].astype(F32)
        own.append(part if j == 0 else part.astype(BF16))
    slab = scattered(own, first)
    parts = [slab[:128]] + [slab[j * 128 : (j + 1) * 128].astype(BF16) for j in range(1, 4)]
    piece = scattered(parts, second)
    return (piece + swap(piece.astype(BF16), "rep").astype(F32)) * scale


def shards(inputs, cotangent, up_weight, down_weight):
    where = jnp.stack([lax.axis_index("z"), lax.axis_index("y")]).astype(jnp.int32)
    scale = 1.0 / math.sqrt(inputs.shape[0] * 256)
    x = jnp.concatenate(gathered(rotate(where, True, inputs), "x"), axis=0)
    c = jnp.concatenate(gathered(rotate(where, False, cotangent), "x"), axis=0)
    up = weight(up_weight, "z", "y")
    down = weight(down_weight.T, "y", "z")
    active = jnp.maximum(jnp.dot(x, up, preferred_element_type=F32), 0.0)
    activation = (active * active).astype(BF16)
    down_grad = grad(c, activation, "z", "y", scale)
    activation_grad = jnp.dot(c, down, preferred_element_type=F32)
    pre_grad = (2.0 * active * activation_grad).astype(BF16)
    up_grad = grad(x, pre_grad, "y", "z", scale)
    back = lax.dot_general(pre_grad, up, (((1,), (1,)), ((), ())), preferred_element_type=F32).astype(BF16)
    parts = [back[j * 128 : (j + 1) * 128] for j in range(4)]
    input_grad = unrotate(where, True, scattered(parts, "x"))
    return input_grad, up_grad, down_grad.T


def solution(mesh):
    torus = Mesh(mesh.devices.reshape(2, 4, 4, 4, 2), ALL)
    return jax.shard_map(
        shards,
        mesh=torus,
        in_specs=(P(ALL, None), P(ALL, None), P(("z", "y"), ("x", "core")), P(("x", "core"), ("z", "y"))),
        out_specs=(P(ALL, None), P(("z", "y"), ("x", "core")), P(("x", "core"), ("z", "y"))),
        check_vma=False,
    )
```

```python
import math

import jax
import jax.numpy as jnp
from jax import lax
from jax.experimental import pallas as pl
from jax.experimental.pallas import tpu as pltpu
from jax.sharding import Mesh
from jax.sharding import PartitionSpec as P


ALL = ("rep", "z", "y", "x", "core")
F32, BF16 = jnp.float32, jnp.bfloat16
VMEM = pl.BlockSpec(memory_space=pltpu.VMEM)
SMEM = pl.BlockSpec(memory_space=pltpu.SMEM)
ANY = pl.BlockSpec(memory_space=pl.ANY)
HBM = pl.BlockSpec(memory_space=pltpu.HBM)
SLABS = ((0, 512), (512, 512), (1024, 256), (1280, 256), (1536, 512))


def shape(*dims, dtype=BF16):
    return jax.ShapeDtypeStruct(dims, dtype)


def cost(flops, size):
    return pl.CostEstimate(flops=flops, bytes_accessed=size, transcendentals=0)


def along_x(v, by):
    return lax.ppermute(v, "x", [(i, (i + by) % 4) for i in range(4)])


def swap(v, axis):
    pairs = [(0, 1), (1, 0)] if isinstance(axis, str) else [(0, 3), (1, 2), (2, 1), (3, 0)]
    return lax.ppermute(v, axis, pairs)


def crossed(v, by, core_of_z):
    pairs = []
    for z in range(8):
        for y in range(4):
            for core in range(2):
                to = ((z + by) % 8, y) if core == core_of_z else (z, (y + by) % 4)
                pairs.append(((z * 4 + y) * 2 + core, (to[0] * 4 + to[1]) * 2 + core))
    return lax.ppermute(v, ("rep", "z", "y", "core"), pairs)


def block_of(at, j, y_major):
    a, b = j // 4, j % 4
    ry, rz = (a, b) if y_major else (b, a)
    return lax.rem(at[0] + rz, 4) * 4 + lax.rem(at[1] + ry, 4)


def prepare(at, inputs, cotangent, up, down):
    def kernel(at, x_ref, c_ref, u_ref, d_ref, xo, co, keep, send):
        down_t = d_ref[...].astype(F32).T.astype(BF16)
        first = at[2] == 0
        keep[...] = jnp.where(first, u_ref[...], down_t)
        send[...] = jnp.where(first, down_t, u_ref[...])
        for j in range(16):
            cols = slice(j * 128, (j + 1) * 128)
            src = pl.multiple_of(block_of(at, j, True) * 128, 128)
            xo[:, cols] = x_ref[:, pl.ds(src, 128)]
            src = pl.multiple_of(block_of(at, j, False) * 128, 128)
            co[:, cols] = c_ref[:, pl.ds(src, 128)]

    return pl.pallas_call(
        kernel,
        out_shape=(shape(128, 2048), shape(128, 2048), shape(128, 512), shape(128, 512)),
        in_specs=[SMEM] + [VMEM] * 4,
        out_specs=(VMEM,) * 4,
        cost_estimate=cost(4_000_000, 3 << 20),
        compiler_params=pltpu.CompilerParams(vmem_limit_bytes=8 << 20),
        name="prepare",
    )(at, inputs, cotangent, up, down)


def join(at, kept, received):
    def kernel(at, k_ref, r_ref, whole, low, high):
        mine = pl.ds(pl.multiple_of(at[2] * 512, 512), 512)
        other = pl.ds(pl.multiple_of((1 - at[2]) * 512, 512), 512)
        for ref, col in ((k_ref, mine), (r_ref, other)):
            whole[:, col] = ref[...]
            low[:, col] = ref[:64]
            high[:, col] = ref[64:]

    return pl.pallas_call(
        kernel,
        out_shape=(shape(128, 1024), shape(64, 1024), shape(64, 1024)),
        in_specs=[SMEM, VMEM, VMEM],
        out_specs=(VMEM,) * 3,
        cost_estimate=cost(1_000_000, 1 << 20),
        compiler_params=pltpu.CompilerParams(vmem_limit_bytes=8 << 20),
        name="join",
    )(at, kept, received)


def stack(r0, r1, r2a, r2b, r3):
    def kernel(a, b, c, d, e, whole, low, high):
        for ref, row in ((a, 0), (b, 128), (c, 256), (d, 320), (e, 384)):
            n = ref.shape[0]
            whole[row : row + n] = ref[...]
            half, r = (low, row) if row < 256 else (high, row - 256)
            half[r : r + n] = ref[...]

    return pl.pallas_call(
        kernel,
        out_shape=(shape(512, 1024), shape(256, 1024), shape(256, 1024)),
        in_specs=[VMEM] * 5,
        out_specs=(VMEM,) * 3,
        cost_estimate=cost(1_000_000, 3 << 20),
        compiler_params=pltpu.CompilerParams(vmem_limit_bytes=8 << 20),
        name="stack",
    )(r0, r1, r2a, r2b, r3)


def forward(at, xs, cs, own, received):
    def kernel(at, *refs):
        x_in, c_in, mine, theirs = refs[0:4], refs[4:8], refs[8:13], refs[13:18]
        xc, bg, u_v, d_v, active, sems = refs[18:]
        first = at[2] == 0

        def slabs(sources, target, base):
            return [
                pltpu.make_async_copy(sources[k], target.at[pl.ds(row, n)], sems.at[base + k])
                for k, (row, n) in enumerate(SLABS)
            ]

        def blocks(sources, which, base):
            return [
                pltpu.make_async_copy(sources[k], xc.at[which, pl.ds(k * 128, 128)], sems.at[base + k])
                for k in range(4)
            ]

        def begin(u_refs, d_refs):
            for copy in slabs(u_refs, u_v, 0) + blocks(x_in, 0, 5) + slabs(d_refs, d_v, 9) + blocks(c_in, 1, 14):
                copy.start()

        @pl.when(first)
        def _():
            begin(mine, theirs)

        @pl.when(jnp.logical_not(first))
        def _():
            begin(theirs, mine)

        for copy in slabs(mine, u_v, 0) + blocks(x_in, 0, 5):
            copy.wait()

        @pl.loop(0, 4)
        def _(n):
            cols = pl.ds(pl.multiple_of(n * 256, 256), 256)
            a = jnp.maximum(jnp.dot(xc[0], u_v[:, cols], preferred_element_type=F32), 0.0)
            active[:, cols] = a
            bg[1, :, cols] = (a * a).astype(BF16)

        for copy in slabs(theirs, d_v, 9) + blocks(c_in, 1, 14):
            copy.wait()

        @pl.loop(0, 4)
        def _(n):
            cols = pl.ds(pl.multiple_of(n * 256, 256), 256)
            activation_grad = jnp.dot(xc[1], d_v[:, cols], preferred_element_type=F32)
            bg[0, :, cols] = (2.0 * active[:, cols] * activation_grad).astype(BF16)

    return pl.pallas_call(
        kernel,
        out_shape=(shape(2, 512, 2048), shape(2, 512, 1024), shape(2048, 1024)),
        in_specs=[SMEM] + [HBM] * 18,
        out_specs=(VMEM,) * 3,
        scratch_shapes=[
            pltpu.VMEM((2048, 1024), BF16),
            pltpu.VMEM((512, 1024), F32),
            pltpu.SemaphoreType.DMA((18,)),
        ],
        compiler_params=pltpu.CompilerParams(vmem_limit_bytes=22 << 20),
        cost_estimate=cost(4 * 512 * 2048 * 1024, 24 << 20),
        name="forward",
    )(at, *xs, *cs, *own, *received)


def product(which, xc, bg, slab, added=None, after=None, split=False, dtype=BF16):
    def kernel(which, x_ref, b_ref, *refs):
        refs = list(refs)
        more = refs.pop(0) if added is not None else None
        if after is not None:
            refs.pop(0)
        out = lax.dot_general(x_ref[0], b_ref[0], (((0,), (0,)), ((), ())), preferred_element_type=F32)
        if more is not None:
            out = out + more[...].astype(F32)
        n = 512 // len(refs)
        for k, o in enumerate(refs):
            o[...] = out[k * n : (k + 1) * n].astype(o.dtype)

    parts = 2 if split else 1
    n = 512 // parts
    in_specs = [
        pl.BlockSpec((1, 512, 512), lambda i, s: (s[0], 0, slab)),
        pl.BlockSpec((1, 512, 512), lambda i, s: (s[0], 0, i)),
    ]
    args = [which, xc, bg]
    if added is not None:
        in_specs.append(pl.BlockSpec((512, 512), lambda i, s: (0, i)))
        args.append(added)
    if after is not None:
        in_specs.append(ANY)
        args.append(after)
    out = pl.pallas_call(
        kernel,
        out_shape=[shape(n, 1024, dtype=dtype)] * parts,
        grid_spec=pltpu.PrefetchScalarGridSpec(
            num_scalar_prefetch=1,
            grid=(2,),
            in_specs=in_specs,
            out_specs=[pl.BlockSpec((n, 512), lambda i, s: (0, i))] * parts,
        ),
        compiler_params=pltpu.CompilerParams(vmem_limit_bytes=14 << 20),
        cost_estimate=cost(2 * 512 * 512 * 1024, 5 << 20),
        name="product",
    )(*args)
    return out if split else out[0]


def backward(bg, up):
    def kernel(b_ref, u_ref, *outs):
        r = lax.dot_general(b_ref[0], u_ref[...], (((1,), (1,)), ((), ())), preferred_element_type=F32)
        for k, o in enumerate(outs):
            o[...] = r[k * 128 : (k + 1) * 128].astype(BF16)

    return pl.pallas_call(
        kernel,
        out_shape=[shape(128, 2048)] * 4,
        grid=(4,),
        in_specs=[pl.BlockSpec((1, 512, 1024), lambda i: (0, 0, 0)), pl.BlockSpec((512, 1024), lambda i: (i, 0))],
        out_specs=[pl.BlockSpec((128, 512), lambda i: (0, i))] * 4,
        compiler_params=pltpu.CompilerParams(vmem_limit_bytes=14 << 20),
        cost_estimate=cost(2 * 512 * 2048 * 1024, 8 << 20),
        name="backward",
    )(bg, up)


def total(at, parts):
    def kernel(at, a, b, c, d, o_ref):
        for j in range(16):
            cols = slice(j * 128, (j + 1) * 128)
            dst = pl.ds(pl.multiple_of(block_of(at, j, True) * 128, 128), 128)
            r = a[:, cols].astype(F32) + b[:, cols].astype(F32) + c[:, cols].astype(F32) + d[:, cols].astype(F32)
            o_ref[:, dst] = r.astype(BF16)

    return pl.pallas_call(
        kernel,
        out_shape=shape(128, 2048),
        in_specs=[SMEM] + [VMEM] * 4,
        out_specs=VMEM,
        cost_estimate=cost(4_000_000, 5 << 19),
        compiler_params=pltpu.CompilerParams(vmem_limit_bytes=8 << 20),
        name="total",
    )(at, *parts)


def sends(g, core_of_z):
    g1, g3, g2a, g2b = g
    return (
        crossed(g2a, 2, core_of_z), crossed(g2b, -2, core_of_z), crossed(g1, 1, core_of_z), crossed(g3, -1, core_of_z)
    )


def added(g0, arrived):
    far_a, far_b, one, three = arrived
    n = far_a.shape[0]
    low = g0[:n] + one[:n].astype(F32) + three[:n].astype(F32) + far_a.astype(F32)
    high = g0[n:] + one[n:].astype(F32) + three[n:].astype(F32) + far_b.astype(F32)
    return low, high


def halves(at, g0, arrived):
    def kernel(at, g, a, b, one, three, mine, rounded, other):
        for here, out in ((at[2], mine), (1 - at[2], other)):
            cols = pl.ds(pl.multiple_of(here * 512, 512), 512)
            for far, row in ((a, 0), (b, 64)):
                rows = pl.ds(row, 64)
                r = g[rows, cols] + one[rows, cols].astype(F32) + three[rows, cols].astype(F32) + far[:, cols].astype(F32)
                out[rows] = r.astype(out.dtype)
                if out is mine:
                    rounded[rows] = r.astype(BF16)

    return pl.pallas_call(
        kernel,
        out_shape=(shape(128, 512, dtype=F32), shape(128, 512), shape(128, 512)),
        in_specs=[SMEM] + [VMEM] * 5,
        out_specs=(VMEM,) * 3,
        cost_estimate=cost(1_000_000, 2 << 20),
        compiler_params=pltpu.CompilerParams(vmem_limit_bytes=8 << 20),
        name="halves",
    )(at, g0, *arrived)


def finish(at, mine, mine_far, other, other_far, scale):
    def kernel(at, a, b, c, d, up, down):
        first = at[2] == 0
        one = (a[...] + b[...].astype(F32)) * scale
        two = (c[...].astype(F32) + d[...].astype(F32)) * scale
        up[...] = jnp.where(first, one, two)
        down[...] = jnp.where(first, two, one).T

    return pl.pallas_call(
        kernel,
        out_shape=(shape(128, 512, dtype=F32), shape(512, 128, dtype=F32)),
        in_specs=[SMEM] + [VMEM] * 4,
        out_specs=(VMEM,) * 2,
        cost_estimate=cost(1_000_000, 1 << 20),
        compiler_params=pltpu.CompilerParams(vmem_limit_bytes=8 << 20),
        name="finish",
    )(at, mine, mine_far, other, other_far)


def step(inputs, cotangent, up_weight, down_weight):
    core = lax.axis_index("core")
    at = jnp.stack([lax.axis_index("z"), lax.axis_index("y"), core]).astype(jnp.int32)
    keep_at, send_at = core.astype(jnp.int32)[None], (1 - core).astype(jnp.int32)[None]
    scale = 1.0 / math.sqrt(inputs.shape[0] * 256)

    x0, c0, kept, sent = prepare(at, inputs, cotangent, up_weight, down_weight)
    received = swap(sent, "core")
    x3, x1 = along_x(x0, 1), along_x(x0, -1)
    c3, c1 = along_x(c0, 1), along_x(c0, -1)
    w, w_low, w_high = join(at, kept, received)
    w2a, w2b, w3, w1 = sends((w, w, w_low, w_high), 0)
    s, s_low, s_high = stack(w, w1, w2a, w2b, w3)
    s2a, s2b, s3, s1 = sends((s, s, s_low, s_high), 1)
    own = (s, s1, s2a, s2b, s3)
    theirs = tuple(swap(v, "core") for v in own)
    x2, c2 = along_x(x3, 1), along_x(c1, -1)

    xc, bg, up = forward(at, (x0, x1, x2, x3), (c0, c1, c2, c3), own, theirs)

    other = [swap(product(send_at, xc, bg, j), "core") for j in (2, 1, 3, 0)]
    back = backward(bg, up)
    b2, b1, b3 = along_x(back[2], 2), along_x(back[1], 1), along_x(back[3], -1)
    g2a, g2b = product(keep_at, xc, bg, 2, other[0], back[0], split=True)
    g1 = product(keep_at, xc, bg, 1, other[1], back[0])
    g3 = product(keep_at, xc, bg, 3, other[2], back[0])
    g0 = product(keep_at, xc, bg, 0, other[3], back[0], dtype=F32)
    low, high = added(g0, sends((g1, g3, g2a, g2b), 1))
    arrived = sends((low[128:].astype(BF16), high[128:].astype(BF16), high[:64].astype(BF16), high[64:128].astype(BF16)), 0)
    mine, rounded, theirs = halves(at, low[:128], arrived)
    far_mine = swap(rounded, "rep")
    near = swap(theirs, "core")
    far = swap(theirs, ("rep", "core"))
    up_grad, down_grad = finish(at, mine, far_mine, near, far, scale)

    return total(at, (back[0], b2, b1, b3)), up_grad, down_grad


def solution(mesh):
    torus = Mesh(mesh.devices.reshape(2, 4, 4, 4, 2), ALL)
    return jax.shard_map(
        step,
        mesh=torus,
        in_specs=(P(ALL, None), P(ALL, None), P(("z", "y"), ("x", "core")), P(("x", "core"), ("z", "y"))),
        out_specs=(P(ALL, None), P(("z", "y"), ("x", "core")), P(("x", "core"), ("z", "y"))),
        check_vma=False,
    )
```

```python
import math

import jax
import jax.numpy as jnp
from jax import lax
from jax.experimental import pallas as pl
from jax.experimental.pallas import tpu as pltpu
from jax.sharding import Mesh
from jax.sharding import PartitionSpec as P


ALL = ("rep", "z", "y", "x", "core")
F32, BF16 = jnp.float32, jnp.bfloat16
VMEM = pl.BlockSpec(memory_space=pltpu.VMEM)
SMEM = pl.BlockSpec(memory_space=pltpu.SMEM)
ANY = pl.BlockSpec(memory_space=pl.ANY)
HBM = pl.BlockSpec(memory_space=pltpu.HBM)


def shape(*dims, dtype=BF16):
    return jax.ShapeDtypeStruct(dims, dtype)


def cost(flops, size):
    return pl.CostEstimate(flops=flops, bytes_accessed=size, transcendentals=0)


def along_x(v, by):
    return lax.ppermute(v, "x", [(i, (i + by) % 4) for i in range(4)])


def swap(v, axis):
    pairs = [(0, 1), (1, 0)] if isinstance(axis, str) else [(0, 3), (1, 2), (2, 1), (3, 0)]
    return lax.ppermute(v, axis, pairs)


def crossed(v, by, core_of_z):
    pairs = []
    for z in range(8):
        for y in range(4):
            for core in range(2):
                step = -2 if by == 2 and z % 2 == 0 else by
                to = ((z + step) % 8, y) if core == core_of_z else (z, (y + by) % 4)
                pairs.append(((z * 4 + y) * 2 + core, (to[0] * 4 + to[1]) * 2 + core))
    return lax.ppermute(v, ("rep", "z", "y", "core"), pairs)


def block_of(at, j, y_major):
    a, b = j // 4, j % 4
    ry, rz = (a, b) if y_major else (b, a)
    return lax.rem(at[0] + rz, 4) * 4 + lax.rem(at[1] + ry, 4)


def prepare(at, inputs, cotangent, up, down):
    def kernel(at, x_in, c_in, u_in, d_in, xo, co, keep, send, x_ref, c_ref, u_ref, d_ref, sems):
        pairs = ((x_in, x_ref), (u_in, u_ref), (d_in, d_ref), (c_in, c_ref))
        copies = [pltpu.make_async_copy(a, b, sems.at[k]) for k, (a, b) in enumerate(pairs)]
        for copy in copies:
            copy.start()
        copies[0].wait()
        for j in range(16):
            src = pl.multiple_of(block_of(at, j, True) * 128, 128)
            xo[:, j * 128 : (j + 1) * 128] = x_ref[:, pl.ds(src, 128)]
        copies[1].wait()
        copies[2].wait()
        down_t = d_ref[...].astype(F32).T.astype(BF16)
        first = at[2] == 0
        keep[...] = jnp.where(first, u_ref[...], down_t)
        send[...] = jnp.where(first, down_t, u_ref[...])
        copies[3].wait()
        for j in range(16):
            src = pl.multiple_of(block_of(at, j, False) * 128, 128)
            co[:, j * 128 : (j + 1) * 128] = c_ref[:, pl.ds(src, 128)]

    return pl.pallas_call(
        kernel,
        out_shape=(shape(128, 2048), shape(128, 2048), shape(128, 512), shape(128, 512)),
        in_specs=[SMEM] + [HBM] * 4,
        out_specs=(VMEM,) * 4,
        scratch_shapes=[
            pltpu.VMEM((128, 2048), BF16),
            pltpu.VMEM((128, 2048), BF16),
            pltpu.VMEM((128, 512), BF16),
            pltpu.VMEM((512, 128), BF16),
            pltpu.SemaphoreType.DMA((4,)),
        ],
        cost_estimate=cost(4_000_000, 3 << 20),
        name="prepare",
    )(at, inputs, cotangent, up, down)


def join(at, kept, received):
    def kernel(at, k_ref, r_ref, whole):
        whole[:, pl.ds(pl.multiple_of(at[2] * 512, 512), 512)] = k_ref[...]
        whole[:, pl.ds(pl.multiple_of((1 - at[2]) * 512, 512), 512)] = r_ref[...]

    return pl.pallas_call(
        kernel,
        out_shape=shape(128, 1024),
        in_specs=[SMEM, VMEM, VMEM],
        out_specs=VMEM,
        cost_estimate=cost(1_000_000, 1 << 19),
        compiler_params=pltpu.CompilerParams(vmem_limit_bytes=8 << 20),
        name="join",
    )(at, kept, received)


def stack(*parts):
    def kernel(*refs):
        for k, ref in enumerate(refs[:4]):
            refs[4][k * 128 : (k + 1) * 128] = ref[...]

    return pl.pallas_call(
        kernel,
        out_shape=shape(512, 1024),
        in_specs=[VMEM] * 4,
        out_specs=VMEM,
        cost_estimate=cost(1_000_000, 2 << 20),
        compiler_params=pltpu.CompilerParams(vmem_limit_bytes=8 << 20),
        name="stack",
    )(*parts)


def near_halves(a, b):
    def kernel(a_ref, b_ref, ao, bo):
        ao[...], bo[...] = a_ref[...], b_ref[...]

    return pl.pallas_call(
        kernel,
        out_shape=(shape(256, 1024), shape(256, 1024)),
        grid=(2,),
        in_specs=[pl.BlockSpec((128, 1024), lambda i: (i, 0)), pl.BlockSpec((128, 1024), lambda i: (i + 2, 0))],
        out_specs=[pl.BlockSpec((128, 1024), lambda i: (i, 0))] * 2,
        cost_estimate=cost(1_000_000, 2 << 20),
        compiler_params=pltpu.CompilerParams(vmem_limit_bytes=8 << 20),
        name="near_halves",
    )(a, b)


def rows_into(sources, target, sems, base):
    copies, row = [], 0
    for k, ref in enumerate(sources):
        copies.append(pltpu.make_async_copy(ref, target.at[pl.ds(row, ref.shape[0])], sems.at[base + k]))
        row += ref.shape[0]
    return copies


def started(at, mine, theirs, begin):
    @pl.when(at[2] == 0)
    def _():
        for copy in begin(mine, theirs):
            copy.start()

    @pl.when(at[2] != 0)
    def _():
        for copy in begin(theirs, mine):
            copy.start()


def forward_near(at, xs, cs, own, received):
    def kernel(at, *refs):
        x_in, c_in, mine, theirs = refs[0:3], refs[3:6], refs[6:9], refs[9:12]
        xa, pre, grad, u_a, d_a, sems = refs[12:]

        def begin(u_refs, d_refs):
            return (
                rows_into(u_refs, u_a, sems, 0)
                + rows_into(x_in, xa.at[0], sems, 3)
                + rows_into(d_refs, d_a, sems, 6)
                + rows_into(c_in, xa.at[1], sems, 9)
            )

        started(at, mine, theirs, begin)
        copies = begin(mine, theirs)
        for which, w, out in ((0, u_a, pre), (1, d_a, grad)):
            for copy in copies[which * 6 : which * 6 + 6]:
                copy.wait()

            @pl.loop(0, 4)
            def _(n):
                cols = pl.ds(pl.multiple_of(n * 256, 256), 256)
                out[:, cols] = jnp.dot(xa[which, :, :1024], w[:1024, cols], preferred_element_type=F32) + jnp.dot(
                    xa[which, :, 1536:], w[1024:, cols], preferred_element_type=F32
                )

    return pl.pallas_call(
        kernel,
        out_shape=(
            shape(2, 384, 2048),
            shape(384, 1024, dtype=F32),
            shape(384, 1024, dtype=F32),
            shape(1536, 1024),
            shape(1536, 1024),
        ),
        in_specs=[SMEM] + [HBM] * 12,
        out_specs=(VMEM,) * 5,
        scratch_shapes=[pltpu.SemaphoreType.DMA((12,))],
        compiler_params=pltpu.CompilerParams(vmem_limit_bytes=18 << 20),
        cost_estimate=cost(4 * 384 * 1536 * 1024, 18 << 20),
        name="forward_near",
    )(at, *xs, *cs, *own, *received)


def forward_far(at, near, x2, c2, own, received):
    def kernel(at, xa, pre, grad, u_a, d_a, x_in, c_in, m0, m1, t0, t1, xb, bga, bgb, u_b, d_b, sems):
        def begin(u_refs, d_refs):
            return (
                rows_into((x_in,), xb.at[0], sems, 0)
                + rows_into((c_in,), xb.at[1], sems, 1)
                + rows_into(u_refs, u_b, sems, 2)
                + rows_into(d_refs, d_b, sems, 4)
            )

        started(at, (m0, m1), (t0, t1), begin)
        for copy in begin((m0, m1), (t0, t1)):
            copy.wait()

        def last(which, near_w, far_w, cols):
            return (
                jnp.dot(xb[which, :, :1024], near_w[:1024, cols], preferred_element_type=F32)
                + jnp.dot(xb[which, :, 1024:1536], far_w[:, cols], preferred_element_type=F32)
                + jnp.dot(xb[which, :, 1536:], near_w[1024:, cols], preferred_element_type=F32)
            )

        def store(out, active, activation_grad, cols):
            active = jnp.maximum(active, 0.0)
            out[1, :, cols] = (active * active).astype(BF16)
            out[0, :, cols] = (2.0 * active * activation_grad).astype(BF16)

        @pl.loop(0, 4)
        def _(n):
            cols = pl.ds(pl.multiple_of(n * 256, 256), 256)
            a = pre[:, cols] + jnp.dot(xa[0, :, 1024:1536], u_b[:, cols], preferred_element_type=F32)
            g = grad[:, cols] + jnp.dot(xa[1, :, 1024:1536], d_b[:, cols], preferred_element_type=F32)
            store(bga, a, g, cols)
            store(bgb, last(0, u_a, u_b, cols), last(1, d_a, d_b, cols), cols)

    return pl.pallas_call(
        kernel,
        out_shape=(shape(2, 128, 2048), shape(2, 384, 1024), shape(2, 128, 1024), shape(512, 1024)),
        in_specs=[SMEM] + [VMEM] * 5 + [HBM] * 6,
        out_specs=(VMEM,) * 4,
        scratch_shapes=[pltpu.VMEM((512, 1024), BF16), pltpu.SemaphoreType.DMA((6,))],
        compiler_params=pltpu.CompilerParams(vmem_limit_bytes=10 << 20),
        cost_estimate=cost(4 * 1024 * (512 * 2048 - 384 * 1536), 6 << 20),
        name="forward_far",
    )(at, *near, x2, c2, *own, *received)


def product(core, keep, tokens, slab, added=None, dtype=BF16):
    def which(s):
        return s[0] if keep else 1 - s[0]

    def kernel(core, xa, ba, xb, bb, *refs):
        refs = list(refs)
        more = refs.pop(0) if added is not None else None
        out = lax.dot_general(xa[0], ba[0], (((0,), (0,)), ((), ())), preferred_element_type=F32)
        out = out + lax.dot_general(xb[0], bb[0], (((0,), (0,)), ((), ())), preferred_element_type=F32)
        if more is not None:
            out = out + more[...].astype(F32)
        refs[0][...] = out.astype(dtype)

    in_specs = []
    for rows in (384, 128):
        in_specs.append(pl.BlockSpec((1, rows, 512), lambda i, s: (which(s), 0, slab)))
        in_specs.append(pl.BlockSpec((1, rows, 512), lambda i, s: (which(s), 0, i)))
    args = [core, *tokens]
    if added is not None:
        in_specs.append(pl.BlockSpec((512, 512), lambda i, s: (0, i)))
        args.append(added)
    return pl.pallas_call(
        kernel,
        out_shape=shape(512, 1024, dtype=dtype),
        grid_spec=pltpu.PrefetchScalarGridSpec(
            num_scalar_prefetch=1,
            grid=(2,),
            in_specs=in_specs,
            out_specs=pl.BlockSpec((512, 512), lambda i, s: (0, i)),
        ),
        compiler_params=pltpu.CompilerParams(vmem_limit_bytes=12 << 20),
        cost_estimate=cost(2 * 512 * 512 * 1024, 5 << 20),
        name="product",
    )(*args)


def backward(bga, bgb, u_a, u_b):
    def kernel(a_ref, b_ref, ua_ref, ub_ref, *outs):
        def write(u):
            near = lax.dot_general(a_ref[0], u, (((1,), (1,)), ((), ())), preferred_element_type=F32)
            for k, o in enumerate(outs[:3]):
                o[...] = near[k * 128 : (k + 1) * 128].astype(BF16)
            far = lax.dot_general(b_ref[0], u, (((1,), (1,)), ((), ())), preferred_element_type=F32)
            outs[3][...] = far.astype(BF16)

        @pl.when(pl.program_id(0) < 3)
        def _():
            write(ua_ref[...])

        @pl.when(pl.program_id(0) == 3)
        def _():
            write(ub_ref[...])

    return pl.pallas_call(
        kernel,
        out_shape=[shape(128, 2048)] * 4,
        grid=(4,),
        in_specs=[
            pl.BlockSpec((1, 384, 1024), lambda i: (0, 0, 0)),
            pl.BlockSpec((1, 128, 1024), lambda i: (0, 0, 0)),
            pl.BlockSpec((512, 1024), lambda i: (jnp.minimum(i, 2), 0)),
            pl.BlockSpec((512, 1024), lambda i: (0, 0)),
        ],
        out_specs=[pl.BlockSpec((128, 512), lambda i: (0, i + jnp.where(i == 2, 1, 0) - jnp.where(i == 3, 1, 0)))] * 4,
        compiler_params=pltpu.CompilerParams(vmem_limit_bytes=14 << 20),
        cost_estimate=cost(2 * 512 * 2048 * 1024, 8 << 20),
        name="backward",
    )(bga, bgb, u_a, u_b)


def total(at, parts):
    def kernel(at, a, b, c, d, o_ref):
        for j in range(16):
            cols = slice(j * 128, (j + 1) * 128)
            dst = pl.ds(pl.multiple_of(block_of(at, j, True) * 128, 128), 128)
            r = a[:, cols].astype(F32) + b[:, cols].astype(F32) + c[:, cols].astype(F32) + d[:, cols].astype(F32)
            o_ref[:, dst] = r.astype(BF16)

    return pl.pallas_call(
        kernel,
        out_shape=shape(128, 2048),
        in_specs=[SMEM] + [VMEM] * 4,
        out_specs=VMEM,
        cost_estimate=cost(4_000_000, 5 << 19),
        compiler_params=pltpu.CompilerParams(vmem_limit_bytes=8 << 20),
        name="total",
    )(at, *parts)


def sends(g, core_of_z):
    g1, g2, g3 = g
    two = crossed(g2, 2, core_of_z)
    return crossed(g1, 1, core_of_z), two, crossed(g3, -1, core_of_z)


def added(g0, arrived):
    a, b, c = arrived
    return g0 + a.astype(F32) + b.astype(F32) + c.astype(F32)


def halves(at, g0, arrived):
    def kernel(at, g, a, b, c, mine, rounded, other):
        for here, out in ((at[2], mine), (1 - at[2], other)):
            cols = pl.ds(pl.multiple_of(here * 512, 512), 512)
            r = g[:, cols] + a[:, cols].astype(F32) + b[:, cols].astype(F32) + c[:, cols].astype(F32)
            out[...] = r.astype(out.dtype)
            if out is mine:
                rounded[...] = r.astype(BF16)

    return pl.pallas_call(
        kernel,
        out_shape=(shape(128, 512, dtype=F32), shape(128, 512), shape(128, 512)),
        in_specs=[SMEM] + [VMEM] * 4,
        out_specs=(VMEM,) * 3,
        cost_estimate=cost(1_000_000, 2 << 20),
        compiler_params=pltpu.CompilerParams(vmem_limit_bytes=8 << 20),
        name="halves",
    )(at, g0, *arrived)


def finish(at, mine, mine_far, other, other_far, scale):
    def kernel(at, a, b, c, d, up, down):
        first = at[2] == 0
        one = (a[...] + b[...].astype(F32)) * scale
        two = (c[...].astype(F32) + d[...].astype(F32)) * scale
        up[...] = jnp.where(first, one, two)
        down[...] = jnp.where(first, two, one).T

    return pl.pallas_call(
        kernel,
        out_shape=(shape(128, 512, dtype=F32), shape(512, 128, dtype=F32)),
        in_specs=[SMEM] + [VMEM] * 4,
        out_specs=(VMEM,) * 2,
        cost_estimate=cost(1_000_000, 1 << 20),
        compiler_params=pltpu.CompilerParams(vmem_limit_bytes=8 << 20),
        name="finish",
    )(at, mine, mine_far, other, other_far)


def step(inputs, cotangent, up_weight, down_weight):
    core = lax.axis_index("core")
    at = jnp.stack([lax.axis_index("z"), lax.axis_index("y"), core]).astype(jnp.int32)
    here = core.astype(jnp.int32)[None]
    scale = 1.0 / math.sqrt(inputs.shape[0] * 256)

    x0, c0, kept, sent = prepare(at, inputs, cotangent, up_weight, down_weight)
    received = swap(sent, "core")
    x3, c1 = along_x(x0, 1), along_x(c0, -1)
    c3, x1 = along_x(c0, 1), along_x(x0, -1)
    w = join(at, kept, received)
    w3, w2, w1 = sends((w, w, w), 0)
    s0 = stack(w, w1, w2, w3)
    s3, s1 = crossed(s0, 1, 1), crossed(s0, -1, 1)
    h3, h1 = near_halves(s3, s1)
    far = crossed(h3, 1, 1), crossed(h1, -1, 1)
    x2, c2 = along_x(x3, 1), along_x(c1, -1)
    own = (s0, s1, s3)
    theirs = tuple(swap(v, "core") for v in own)
    near = forward_near(at, (x0, x1, x3), (c0, c1, c3), own, theirs)
    xb, bga, bgb, u_b = forward_far(at, near, x2, c2, far, (swap(far[0], "core"), swap(far[1], "core")))
    xa, u_a = near[0], near[3]
    tokens = (xa, bga, xb, bgb)

    o2 = swap(product(here, False, tokens, 2), "core")
    o1 = swap(product(here, False, tokens, 1), "core")
    o3 = swap(product(here, False, tokens, 3), "core")
    g2 = product(here, True, tokens, 2, o2)
    g1 = product(here, True, tokens, 1, o1)
    g3 = product(here, True, tokens, 3, o3)
    o0 = swap(product(here, False, tokens, 0), "core")
    back0, back1, back3, back2 = backward(bga, bgb, u_a, u_b)
    b2, b1, b3 = along_x(back2, 2), along_x(back1, 1), along_x(back3, -1)
    g0 = product(here, True, tokens, 0, o0, dtype=F32)
    g = added(g0, sends((g1, g2, g3), 1)).reshape(4, 128, 1024)
    arrived = sends(tuple(g[k].astype(BF16) for k in (1, 2, 3)), 0)
    mine, rounded, theirs = halves(at, g[0], arrived)
    far_mine = swap(rounded, "rep")
    near = swap(theirs, "core")
    far = swap(theirs, ("rep", "core"))
    up_grad, down_grad = finish(at, mine, far_mine, near, far, scale)

    return total(at, (back0, b2, b1, b3)), up_grad, down_grad


def solution(mesh):
    torus = Mesh(mesh.devices.reshape(2, 4, 4, 4, 2), ALL)
    return jax.shard_map(
        step,
        mesh=torus,
        in_specs=(P(ALL, None), P(ALL, None), P(("z", "y"), ("x", "core")), P(("x", "core"), ("z", "y"))),
        out_specs=(P(ALL, None), P(("z", "y"), ("x", "core")), P(("x", "core"), ("z", "y"))),
        check_vma=False,
    )
```

```python
import math

import jax
import jax.numpy as jnp
from jax import lax
from jax.experimental import pallas as pl
from jax.experimental.pallas import tpu as pltpu
from jax.sharding import Mesh
from jax.sharding import PartitionSpec as P


ALL = ("rep", "z", "y", "x", "core")
F32, BF16 = jnp.float32, jnp.bfloat16
VMEM = pl.BlockSpec(memory_space=pltpu.VMEM)
HBM = pl.BlockSpec(memory_space=pltpu.HBM)


def shape(*dims, dtype=BF16):
    return jax.ShapeDtypeStruct(dims, dtype)


def cost(flops, size):
    return pl.CostEstimate(flops=flops, bytes_accessed=size, transcendentals=0)


def along_x(v, by):
    return lax.ppermute(v, "x", [(i, (i + by) % 4) for i in range(4)])


def swap(v, axis):
    pairs = [(0, 1), (1, 0)] if isinstance(axis, str) else [(0, 3), (1, 2), (2, 1), (3, 0)]
    return lax.ppermute(v, axis, pairs)


def crossed(v, by, core_of_z):
    pairs = []
    for z in range(8):
        for y in range(4):
            for core in range(2):
                step = -2 if by == 2 and z % 2 == 0 else by
                to = ((z + step) % 8, y) if core == core_of_z else (z, (y + by) % 4)
                pairs.append(((z * 4 + y) * 2 + core, (to[0] * 4 + to[1]) * 2 + core))
    return lax.ppermute(v, ("rep", "z", "y", "core"), pairs)


def block_of(j, y_major):
    a, b = j // 4, j % 4
    ry, rz = (a, b) if y_major else (b, a)
    return lax.rem(lax.axis_index("z") + rz, 4) * 4 + lax.rem(lax.axis_index("y") + ry, 4)


def prepare_weights(up, down):
    def kernel(u_in, d_in, keep, send, u_ref, d_ref, sems):
        copies = [pltpu.make_async_copy(u_in, u_ref, sems.at[0]), pltpu.make_async_copy(d_in, d_ref, sems.at[1])]
        for copy in copies:
            copy.start()
        for copy in copies:
            copy.wait()
        down_t = d_ref[...].astype(F32).T.astype(BF16)
        first = lax.axis_index("core") == 0
        keep[...] = jnp.where(first, u_ref[...], down_t)
        send[...] = jnp.where(first, down_t, u_ref[...])

    return pl.pallas_call(
        kernel,
        out_shape=(shape(128, 512), shape(128, 512)),
        in_specs=[HBM] * 2,
        out_specs=(VMEM,) * 2,
        scratch_shapes=[
            pltpu.VMEM((128, 512), BF16),
            pltpu.VMEM((512, 128), BF16),
            pltpu.SemaphoreType.DMA((2,)),
        ],
        cost_estimate=cost(2_000_000, 1 << 19),
        name="prepare_weights",
    )(up, down)


def prepare_tokens(inputs, cotangent):
    def kernel(x_in, c_in, xo, co, x_ref, c_ref, sems):
        copies = [pltpu.make_async_copy(x_in, x_ref, sems.at[0]), pltpu.make_async_copy(c_in, c_ref, sems.at[1])]
        for copy in copies:
            copy.start()
        for copy, ref, out, y_major in zip(copies, (x_ref, c_ref), (xo, co), (True, False)):
            copy.wait()
            for j in range(16):
                src = pl.multiple_of(block_of(j, y_major) * 128, 128)
                out[:, j * 128 : (j + 1) * 128] = ref[:, pl.ds(src, 128)]

    return pl.pallas_call(
        kernel,
        out_shape=(shape(128, 2048), shape(128, 2048)),
        in_specs=[HBM] * 2,
        out_specs=(VMEM,) * 2,
        scratch_shapes=[
            pltpu.VMEM((128, 2048), BF16),
            pltpu.VMEM((128, 2048), BF16),
            pltpu.SemaphoreType.DMA((2,)),
        ],
        cost_estimate=cost(4_000_000, 2 << 20),
        name="prepare_tokens",
    )(inputs, cotangent)


def join(kept, received):
    def kernel(k_ref, r_ref, whole):
        core = lax.axis_index("core")
        whole[:, pl.ds(pl.multiple_of(core * 512, 512), 512)] = k_ref[...]
        whole[:, pl.ds(pl.multiple_of((1 - core) * 512, 512), 512)] = r_ref[...]

    return pl.pallas_call(
        kernel,
        out_shape=shape(128, 1024),
        in_specs=[VMEM, VMEM],
        out_specs=VMEM,
        cost_estimate=cost(1_000_000, 1 << 19),
        compiler_params=pltpu.CompilerParams(vmem_limit_bytes=8 << 20),
        name="join",
    )(kept, received)


def stack(*parts):
    def kernel(*refs):
        for k, ref in enumerate(refs[:4]):
            refs[4][k * 128 : (k + 1) * 128] = ref[...]

    return pl.pallas_call(
        kernel,
        out_shape=shape(512, 1024),
        in_specs=[VMEM] * 4,
        out_specs=VMEM,
        cost_estimate=cost(1_000_000, 2 << 20),
        compiler_params=pltpu.CompilerParams(vmem_limit_bytes=8 << 20),
        name="stack",
    )(*parts)


def near_halves(a, b):
    def kernel(a_ref, b_ref, ao, bo):
        ao[...], bo[...] = a_ref[...], b_ref[...]

    return pl.pallas_call(
        kernel,
        out_shape=(shape(256, 1024), shape(256, 1024)),
        grid=(2,),
        in_specs=[pl.BlockSpec((128, 1024), lambda i: (i, 0)), pl.BlockSpec((128, 1024), lambda i: (i + 2, 0))],
        out_specs=[pl.BlockSpec((128, 1024), lambda i: (i, 0))] * 2,
        cost_estimate=cost(1_000_000, 2 << 20),
        compiler_params=pltpu.CompilerParams(vmem_limit_bytes=8 << 20),
        name="near_halves",
    )(a, b)


def rows_into(sources, target, sems, base):
    copies, row = [], 0
    for k, ref in enumerate(sources):
        copies.append(pltpu.make_async_copy(ref, target.at[pl.ds(row, ref.shape[0])], sems.at[base + k]))
        row += ref.shape[0]
    return copies


def started(mine, theirs, begin):
    first = lax.axis_index("core") == 0

    @pl.when(first)
    def _():
        for copy in begin(mine, theirs):
            copy.start()

    @pl.when(jnp.logical_not(first))
    def _():
        for copy in begin(theirs, mine):
            copy.start()


def forward_near(xs, cs, own, received):
    def kernel(*refs):
        x_in, c_in, mine, theirs = refs[0:2], refs[2:4], refs[4:7], refs[7:10]
        xa, pre, grad, u_a, d_a, sems = refs[10:]

        def begin(u_refs, d_refs):
            return (
                rows_into(u_refs, u_a, sems, 0)
                + rows_into(x_in, xa.at[0], sems, 3)
                + rows_into(d_refs, d_a, sems, 5)
                + rows_into(c_in, xa.at[1], sems, 8)
            )

        started(mine, theirs, begin)
        copies = begin(mine, theirs)
        for which, w, out in ((0, u_a, pre), (1, d_a, grad)):
            for copy in copies[which * 5 : which * 5 + 5]:
                copy.wait()

            @pl.loop(0, 4)
            def _(n):
                cols = pl.ds(pl.multiple_of(n * 256, 256), 256)
                out[:, cols] = jnp.dot(xa[which, :, :1024], w[:1024, cols], preferred_element_type=F32) + jnp.dot(
                    xa[which, :, 1536:], w[1024:, cols], preferred_element_type=F32
                )

    return pl.pallas_call(
        kernel,
        out_shape=(
            shape(2, 256, 2048),
            shape(256, 1024, dtype=F32),
            shape(256, 1024, dtype=F32),
            shape(1536, 1024),
            shape(1536, 1024),
        ),
        in_specs=[HBM] * 10,
        out_specs=(VMEM,) * 5,
        scratch_shapes=[pltpu.SemaphoreType.DMA((10,))],
        compiler_params=pltpu.CompilerParams(vmem_limit_bytes=16 << 20),
        cost_estimate=cost(4 * 256 * 1536 * 1024, 18 << 20),
        name="forward_near",
    )(*xs, *cs, *own, *received)


def forward_far(near, xs, cs, own, received):
    def kernel(xa, pre, grad, u_a, d_a, x3, x2, c3, c2, m0, m1, t0, t1, xb, bga, bgb, u_b, d_b, sems):
        def begin(u_refs, d_refs):
            return (
                rows_into(u_refs, u_b, sems, 0)
                + rows_into(d_refs, d_b, sems, 2)
                + rows_into((x3, x2), xb.at[0], sems, 4)
                + rows_into((c3, c2), xb.at[1], sems, 6)
            )

        started((m0, m1), (t0, t1), begin)
        copies = begin((m0, m1), (t0, t1))

        def last(which, near_w, far_w, cols):
            return (
                jnp.dot(xb[which, :, :1024], near_w[:1024, cols], preferred_element_type=F32)
                + jnp.dot(xb[which, :, 1024:1536], far_w[:, cols], preferred_element_type=F32)
                + jnp.dot(xb[which, :, 1536:], near_w[1024:, cols], preferred_element_type=F32)
            )

        def store(out, active, activation_grad, cols):
            active = jnp.maximum(active, 0.0)
            out[1, :, cols] = (active * active).astype(BF16)
            out[0, :, cols] = (2.0 * active * activation_grad).astype(BF16)

        for copy in copies[:4]:
            copy.wait()

        @pl.loop(0, 4)
        def _(n):
            cols = pl.ds(pl.multiple_of(n * 256, 256), 256)
            a = pre[:, cols] + jnp.dot(xa[0, :, 1024:1536], u_b[:, cols], preferred_element_type=F32)
            g = grad[:, cols] + jnp.dot(xa[1, :, 1024:1536], d_b[:, cols], preferred_element_type=F32)
            store(bga, a, g, cols)

        for copy in copies[4:]:
            copy.wait()

        @pl.loop(0, 4)
        def _(n):
            cols = pl.ds(pl.multiple_of(n * 256, 256), 256)
            store(bgb, last(0, u_a, u_b, cols), last(1, d_a, d_b, cols), cols)

    return pl.pallas_call(
        kernel,
        out_shape=(shape(2, 256, 2048), shape(2, 256, 1024), shape(2, 256, 1024), shape(512, 1024)),
        in_specs=[VMEM] * 5 + [HBM] * 8,
        out_specs=(VMEM,) * 4,
        scratch_shapes=[pltpu.VMEM((512, 1024), BF16), pltpu.SemaphoreType.DMA((8,))],
        compiler_params=pltpu.CompilerParams(vmem_limit_bytes=12 << 20),
        cost_estimate=cost(4 * 1024 * (512 * 2048 - 256 * 1536), 6 << 20),
        name="forward_far",
    )(*near, *xs, *cs, *own, *received)


def product(keep, tokens, slab, added=None, dtype=BF16):
    def kernel(xa, ba, xb, bb, *refs):
        core = lax.axis_index("core")
        which = core if keep else 1 - core
        rows = pl.ds(slab * 512, 512)

        @pl.loop(0, 2)
        def _(n):
            cols = pl.ds(pl.multiple_of(n * 512, 512), 512)
            dims = (((0,), (0,)), ((), ()))
            out = lax.dot_general(xa[which, :, rows], ba[which, :, cols], dims, preferred_element_type=F32)
            out = out + lax.dot_general(xb[which, :, rows], bb[which, :, cols], dims, preferred_element_type=F32)
            if added is not None:
                out = out + refs[0][:, cols].astype(F32)
            refs[-1][:, cols] = out.astype(dtype)

    args = [*tokens] + ([] if added is None else [added])
    return pl.pallas_call(
        kernel,
        out_shape=shape(512, 1024, dtype=dtype),
        in_specs=[VMEM] * len(args),
        out_specs=VMEM,
        compiler_params=pltpu.CompilerParams(vmem_limit_bytes=12 << 20),
        cost_estimate=cost(2 * 512 * 512 * 1024, 5 << 20),
        name="product",
    )(*args)


def backward(bga, bgb, u_a, u_b):
    def kernel(a_ref, b_ref, ua_ref, ub_ref, *outs):
        def write(u):
            for k, ref in enumerate((a_ref, b_ref)):
                r = lax.dot_general(ref[0], u, (((1,), (1,)), ((), ())), preferred_element_type=F32).astype(BF16)
                outs[2 * k][...], outs[2 * k + 1][...] = r[:128], r[128:]

        @pl.when(pl.program_id(0) < 3)
        def _():
            write(ua_ref[...])

        @pl.when(pl.program_id(0) == 3)
        def _():
            write(ub_ref[...])

    return pl.pallas_call(
        kernel,
        out_shape=[shape(128, 2048)] * 4,
        grid=(4,),
        in_specs=[
            pl.BlockSpec((1, 256, 1024), lambda i: (0, 0, 0)),
            pl.BlockSpec((1, 256, 1024), lambda i: (0, 0, 0)),
            pl.BlockSpec((512, 1024), lambda i: (jnp.minimum(i, 2), 0)),
            pl.BlockSpec((512, 1024), lambda i: (0, 0)),
        ],
        out_specs=[pl.BlockSpec((128, 512), lambda i: (0, i + jnp.where(i == 2, 1, 0) - jnp.where(i == 3, 1, 0)))] * 4,
        compiler_params=pltpu.CompilerParams(vmem_limit_bytes=14 << 20),
        cost_estimate=cost(2 * 512 * 2048 * 1024, 8 << 20),
        name="backward",
    )(bga, bgb, u_a, u_b)


def total(parts):
    def kernel(a, b, c, d, o_ref):
        for j in range(16):
            cols = slice(j * 128, (j + 1) * 128)
            dst = pl.ds(pl.multiple_of(block_of(j, True) * 128, 128), 128)
            r = a[:, cols].astype(F32) + b[:, cols].astype(F32) + c[:, cols].astype(F32) + d[:, cols].astype(F32)
            o_ref[:, dst] = r.astype(BF16)

    return pl.pallas_call(
        kernel,
        out_shape=shape(128, 2048),
        in_specs=[VMEM] * 4,
        out_specs=VMEM,
        cost_estimate=cost(4_000_000, 5 << 19),
        compiler_params=pltpu.CompilerParams(vmem_limit_bytes=8 << 20),
        name="total",
    )(*parts)


def sends(g, core_of_z):
    g1, g2, g3 = g
    two = crossed(g2, 2, core_of_z)
    return crossed(g1, 1, core_of_z), two, crossed(g3, -1, core_of_z)


def added(g0, arrived):
    a, b, c = arrived
    return g0 + a.astype(F32) + b.astype(F32) + c.astype(F32)


def halves(g0, arrived):
    def kernel(g, a, b, c, mine, rounded, other):
        core = lax.axis_index("core")
        for here, out in ((core, mine), (1 - core, other)):
            cols = pl.ds(pl.multiple_of(here * 512, 512), 512)
            r = g[:, cols] + a[:, cols].astype(F32) + b[:, cols].astype(F32) + c[:, cols].astype(F32)
            out[...] = r.astype(out.dtype)
            if out is mine:
                rounded[...] = r.astype(BF16)

    return pl.pallas_call(
        kernel,
        out_shape=(shape(128, 512, dtype=F32), shape(128, 512), shape(128, 512)),
        in_specs=[VMEM] * 4,
        out_specs=(VMEM,) * 3,
        cost_estimate=cost(1_000_000, 2 << 20),
        compiler_params=pltpu.CompilerParams(vmem_limit_bytes=8 << 20),
        name="halves",
    )(g0, *arrived)


def finish(mine, mine_far, other, other_far, scale):
    def kernel(a, b, c, d, up, down):
        first = lax.axis_index("core") == 0
        one = (a[...] + b[...].astype(F32)) * scale
        two = (c[...].astype(F32) + d[...].astype(F32)) * scale
        up[...] = jnp.where(first, one, two)
        down[...] = jnp.where(first, two, one).T

    return pl.pallas_call(
        kernel,
        out_shape=(shape(128, 512, dtype=F32), shape(512, 128, dtype=F32)),
        in_specs=[VMEM] * 4,
        out_specs=(VMEM,) * 2,
        cost_estimate=cost(1_000_000, 1 << 20),
        compiler_params=pltpu.CompilerParams(vmem_limit_bytes=8 << 20),
        name="finish",
    )(mine, mine_far, other, other_far)


def step(inputs, cotangent, up_weight, down_weight):
    scale = 1.0 / math.sqrt(inputs.shape[0] * 256)

    kept, sent = prepare_weights(up_weight, down_weight)
    received = swap(sent, "core")
    x0, c0 = prepare_tokens(inputs, cotangent)
    x3, c1 = along_x(x0, 1), along_x(c0, -1)
    c3, x1 = along_x(c0, 1), along_x(x0, -1)
    w = join(kept, received)
    w3, w2, w1 = sends((w, w, w), 0)
    s0 = stack(w, w1, w2, w3)
    s3, s1 = crossed(s0, 1, 1), crossed(s0, -1, 1)
    h3, h1 = near_halves(s3, s1)
    far = crossed(h3, 1, 1), crossed(h1, -1, 1)
    x2, c2 = along_x(x3, 1), along_x(c1, -1)
    own = (s0, s1, s3)
    theirs = tuple(swap(v, "core") for v in own)
    near = forward_near((x0, x1), (c0, c1), own, theirs)
    theirs = swap(far[0], "core"), swap(far[1], "core")
    xb, bga, bgb, u_b = forward_far(near, (x3, x2), (c3, c2), far, theirs)
    xa, u_a = near[0], near[3]
    tokens = (xa, bga, xb, bgb)

    o2 = swap(product(False, tokens, 2), "core")
    o1 = swap(product(False, tokens, 1), "core")
    o3 = swap(product(False, tokens, 3), "core")
    g2 = product(True, tokens, 2, o2)
    g1 = product(True, tokens, 1, o1)
    g3 = product(True, tokens, 3, o3)
    o0 = swap(product(False, tokens, 0), "core")
    back0, back1, back3, back2 = backward(bga, bgb, u_a, u_b)
    b2, b1, b3 = along_x(back2, 2), along_x(back1, 1), along_x(back3, -1)
    g0 = product(True, tokens, 0, o0, dtype=F32)
    g = added(g0, sends((g1, g2, g3), 1)).reshape(4, 128, 1024)
    arrived = sends(tuple(g[k].astype(BF16) for k in (1, 2, 3)), 0)
    mine, rounded, theirs = halves(g[0], arrived)
    far_mine = swap(rounded, "rep")
    near = swap(theirs, "core")
    far = swap(theirs, ("rep", "core"))
    up_grad, down_grad = finish(mine, far_mine, near, far, scale)

    return total((back0, b2, b1, b3)), up_grad, down_grad


def solution(mesh):
    torus = Mesh(mesh.devices.reshape(2, 4, 4, 4, 2), ALL)
    return jax.shard_map(
        step,
        mesh=torus,
        in_specs=(P(ALL, None), P(ALL, None), P(("z", "y"), ("x", "core")), P(("x", "core"), ("z", "y"))),
        out_specs=(P(ALL, None), P(("z", "y"), ("x", "core")), P(("x", "core"), ("z", "y"))),
        check_vma=False,
    )
```

```python
import math

import jax
import jax.numpy as jnp
from jax import lax
from jax.experimental import pallas as pl
from jax.experimental.pallas import tpu as pltpu
from jax.sharding import Mesh
from jax.sharding import PartitionSpec as P


ALL = ("rep", "z", "y", "x", "core")
F32, BF16 = jnp.float32, jnp.bfloat16
VMEM = pl.BlockSpec(memory_space=pltpu.VMEM)
HBM = pl.BlockSpec(memory_space=pltpu.HBM)


def shape(*dims, dtype=BF16):
    return jax.ShapeDtypeStruct(dims, dtype)


def cost(flops, size):
    return pl.CostEstimate(flops=flops, bytes_accessed=size, transcendentals=0)


def along_x(v, by):
    return lax.ppermute(v, "x", [(i, (i + by) % 4) for i in range(4)])


def swap(v, axis):
    pairs = [(0, 1), (1, 0)] if isinstance(axis, str) else [(0, 3), (1, 2), (2, 1), (3, 0)]
    return lax.ppermute(v, axis, pairs)


def crossed(v, by, core_of_z):
    pairs = []
    for z in range(8):
        for y in range(4):
            for core in range(2):
                step = -2 if by == 2 and z % 2 == 0 else by
                to = ((z + step) % 8, y) if core == core_of_z else (z, (y + by) % 4)
                pairs.append(((z * 4 + y) * 2 + core, (to[0] * 4 + to[1]) * 2 + core))
    return lax.ppermute(v, ("rep", "z", "y", "core"), pairs)


def block_of(j, y_major):
    a, b = j // 4, j % 4
    ry, rz = (a, b) if y_major else (b, a)
    return lax.rem(lax.axis_index("z") + rz, 4) * 4 + lax.rem(lax.axis_index("y") + ry, 4)


def prepare_weights(up, down):
    def kernel(u_in, d_in, keep, send, u_ref, d_ref, sems):
        copies = [pltpu.make_async_copy(u_in, u_ref, sems.at[0]), pltpu.make_async_copy(d_in, d_ref, sems.at[1])]
        for copy in copies:
            copy.start()
        for copy in copies:
            copy.wait()
        down_t = d_ref[...].astype(F32).T.astype(BF16)
        first = lax.axis_index("core") == 0
        keep[...] = jnp.where(first, u_ref[...], down_t)
        send[...] = jnp.where(first, down_t, u_ref[...])

    return pl.pallas_call(
        kernel,
        out_shape=(shape(128, 512), shape(128, 512)),
        in_specs=[HBM] * 2,
        out_specs=(VMEM,) * 2,
        scratch_shapes=[
            pltpu.VMEM((128, 512), BF16),
            pltpu.VMEM((512, 128), BF16),
            pltpu.SemaphoreType.DMA((2,)),
        ],
        cost_estimate=cost(2_000_000, 1 << 19),
        name="prepare_weights",
    )(up, down)


def prepare_tokens(inputs, cotangent):
    def kernel(x_in, c_in, xo, co, x_ref, c_ref, sems):
        copies = [pltpu.make_async_copy(x_in, x_ref, sems.at[0]), pltpu.make_async_copy(c_in, c_ref, sems.at[1])]
        for copy in copies:
            copy.start()
        for copy, ref, out, y_major in zip(copies, (x_ref, c_ref), (xo, co), (True, False)):
            copy.wait()
            for j in range(16):
                src = pl.multiple_of(block_of(j, y_major) * 128, 128)
                out[:, j * 128 : (j + 1) * 128] = ref[:, pl.ds(src, 128)]

    return pl.pallas_call(
        kernel,
        out_shape=(shape(128, 2048), shape(128, 2048)),
        in_specs=[HBM] * 2,
        out_specs=(VMEM,) * 2,
        scratch_shapes=[
            pltpu.VMEM((128, 2048), BF16),
            pltpu.VMEM((128, 2048), BF16),
            pltpu.SemaphoreType.DMA((2,)),
        ],
        cost_estimate=cost(4_000_000, 2 << 20),
        name="prepare_tokens",
    )(inputs, cotangent)


def join(kept, received):
    def kernel(k_ref, r_ref, whole):
        core = lax.axis_index("core")
        whole[:, pl.ds(pl.multiple_of(core * 512, 512), 512)] = k_ref[...]
        whole[:, pl.ds(pl.multiple_of((1 - core) * 512, 512), 512)] = r_ref[...]

    return pl.pallas_call(
        kernel,
        out_shape=shape(128, 1024),
        in_specs=[VMEM, VMEM],
        out_specs=VMEM,
        cost_estimate=cost(1_000_000, 1 << 19),
        compiler_params=pltpu.CompilerParams(vmem_limit_bytes=8 << 20),
        name="join",
    )(kept, received)


def stack(*parts):
    def kernel(*refs):
        for k, ref in enumerate(refs[:4]):
            refs[4][k * 128 : (k + 1) * 128] = ref[...]

    return pl.pallas_call(
        kernel,
        out_shape=shape(512, 1024),
        in_specs=[VMEM] * 4,
        out_specs=VMEM,
        cost_estimate=cost(1_000_000, 2 << 20),
        compiler_params=pltpu.CompilerParams(vmem_limit_bytes=8 << 20),
        name="stack",
    )(*parts)


def near_halves(a, b):
    def kernel(a_ref, b_ref, ao, bo):
        ao[...], bo[...] = a_ref[...], b_ref[...]

    return pl.pallas_call(
        kernel,
        out_shape=(shape(256, 1024), shape(256, 1024)),
        grid=(2,),
        in_specs=[pl.BlockSpec((128, 1024), lambda i: (i, 0)), pl.BlockSpec((128, 1024), lambda i: (i + 2, 0))],
        out_specs=[pl.BlockSpec((128, 1024), lambda i: (i, 0))] * 2,
        cost_estimate=cost(1_000_000, 2 << 20),
        compiler_params=pltpu.CompilerParams(vmem_limit_bytes=8 << 20),
        name="near_halves",
    )(a, b)


def rows_into(sources, target, sems, base):
    copies, row = [], 0
    for k, ref in enumerate(sources):
        copies.append(pltpu.make_async_copy(ref, target.at[pl.ds(row, ref.shape[0])], sems.at[base + k]))
        row += ref.shape[0]
    return copies


def started(mine, theirs, begin):
    first = lax.axis_index("core") == 0

    @pl.when(first)
    def _():
        for copy in begin(mine, theirs):
            copy.start()

    @pl.when(jnp.logical_not(first))
    def _():
        for copy in begin(theirs, mine):
            copy.start()


def forward_near(xs, cs, own, received):
    def kernel(*refs):
        x_in, c_in, mine, theirs = refs[0:2], refs[2:4], refs[4:7], refs[7:10]
        xa, pre, grad, u_a, d_a, sems = refs[10:]

        def begin(u_refs, d_refs):
            return (
                rows_into(u_refs, u_a, sems, 0)
                + rows_into(x_in, xa.at[0], sems, 3)
                + rows_into(d_refs, d_a, sems, 5)
                + rows_into(c_in, xa.at[1], sems, 8)
            )

        started(mine, theirs, begin)
        copies = begin(mine, theirs)
        for which, w, out in ((0, u_a, pre), (1, d_a, grad)):
            for copy in copies[which * 5 : which * 5 + 5]:
                copy.wait()

            @pl.loop(0, 4)
            def _(n):
                cols = pl.ds(pl.multiple_of(n * 256, 256), 256)
                out[:, cols] = jnp.dot(xa[which, :, :1024], w[:1024, cols], preferred_element_type=F32) + jnp.dot(
                    xa[which, :, 1536:], w[1024:, cols], preferred_element_type=F32
                )

    return pl.pallas_call(
        kernel,
        out_shape=(
            shape(2, 256, 2048),
            shape(256, 1024, dtype=F32),
            shape(256, 1024, dtype=F32),
            shape(1536, 1024),
            shape(1536, 1024),
        ),
        in_specs=[HBM] * 10,
        out_specs=(VMEM,) * 5,
        scratch_shapes=[pltpu.SemaphoreType.DMA((10,))],
        compiler_params=pltpu.CompilerParams(vmem_limit_bytes=16 << 20),
        cost_estimate=cost(4 * 256 * 1536 * 1024, 18 << 20),
        name="forward_near",
    )(*xs, *cs, *own, *received)


def forward_far(near, xs, cs, own, received):
    def kernel(xa, pre, grad, u_a, d_a, x3, x2, c3, c2, m0, m1, t0, t1, xb, bga, bgb, u_b, d_b, sems):
        def begin(u_refs, d_refs):
            return (
                rows_into(u_refs, u_b, sems, 0)
                + rows_into(d_refs, d_b, sems, 2)
                + rows_into((x3, x2), xb.at[0], sems, 4)
                + rows_into((c3, c2), xb.at[1], sems, 6)
            )

        started((m0, m1), (t0, t1), begin)
        copies = begin((m0, m1), (t0, t1))

        def last(which, near_w, far_w, cols):
            return (
                jnp.dot(xb[which, :, :1024], near_w[:1024, cols], preferred_element_type=F32)
                + jnp.dot(xb[which, :, 1024:1536], far_w[:, cols], preferred_element_type=F32)
                + jnp.dot(xb[which, :, 1536:], near_w[1024:, cols], preferred_element_type=F32)
            )

        def store(out, active, activation_grad, cols):
            active = jnp.maximum(active, 0.0)
            out[1, :, cols] = (active * active).astype(BF16)
            out[0, :, cols] = (2.0 * active * activation_grad).astype(BF16)

        for copy in copies[:4]:
            copy.wait()

        @pl.loop(0, 4)
        def _(n):
            cols = pl.ds(pl.multiple_of(n * 256, 256), 256)
            a = pre[:, cols] + jnp.dot(xa[0, :, 1024:1536], u_b[:, cols], preferred_element_type=F32)
            g = grad[:, cols] + jnp.dot(xa[1, :, 1024:1536], d_b[:, cols], preferred_element_type=F32)
            store(bga, a, g, cols)

        for copy in copies[4:]:
            copy.wait()

        @pl.loop(0, 4)
        def _(n):
            cols = pl.ds(pl.multiple_of(n * 256, 256), 256)
            store(bgb, last(0, u_a, u_b, cols), last(1, d_a, d_b, cols), cols)

    return pl.pallas_call(
        kernel,
        out_shape=(shape(2, 256, 2048), shape(2, 256, 1024), shape(2, 256, 1024), shape(512, 1024)),
        in_specs=[VMEM] * 5 + [HBM] * 8,
        out_specs=(VMEM,) * 4,
        scratch_shapes=[pltpu.VMEM((512, 1024), BF16), pltpu.SemaphoreType.DMA((8,))],
        compiler_params=pltpu.CompilerParams(vmem_limit_bytes=12 << 20),
        cost_estimate=cost(4 * 1024 * (512 * 2048 - 256 * 1536), 6 << 20),
        name="forward_far",
    )(*near, *xs, *cs, *own, *received)


DIMS = (((0,), (0,)), ((), ()))


def to_send(tokens, *slabs):
    def kernel(xa, ba, xb, bb, out):
        which = 1 - lax.axis_index("core")

        @pl.loop(0, 2 * len(slabs))
        def _(k):
            part = k // 2
            slab = slabs[0] if len(slabs) == 1 else jnp.where(part == 0, slabs[0], slabs[1])
            rows = pl.ds(pl.multiple_of(slab * 512, 512), 512)
            cols = pl.ds(pl.multiple_of((k % 2) * 512, 512), 512)
            r = lax.dot_general(xa[which, :, rows], ba[which, :, cols], DIMS, preferred_element_type=F32)
            r = r + lax.dot_general(xb[which, :, rows], bb[which, :, cols], DIMS, preferred_element_type=F32)
            out[pl.ds(pl.multiple_of(part * 512, 512), 512), cols] = r.astype(BF16)

    return pl.pallas_call(
        kernel,
        out_shape=shape(512 * len(slabs), 1024),
        in_specs=[VMEM] * 4,
        out_specs=VMEM,
        compiler_params=pltpu.CompilerParams(vmem_limit_bytes=12 << 20),
        cost_estimate=cost(2 * 512 * 512 * 1024 * len(slabs), 5 << 20),
        name="to_send",
    )(*tokens)


def kept_half(tokens, slab, added, row, mine, dtype=BF16):
    def kernel(xa, ba, xb, bb, more, out):
        core = lax.axis_index("core")
        base = (core if mine else 1 - core) * 512
        rows = pl.ds(slab * 512, 512)

        @pl.loop(0, 2)
        def _(n):
            cols = pl.ds(pl.multiple_of(base + n * 256, 256), 256)
            r = lax.dot_general(xa[core, :, rows], ba[core, :, cols], DIMS, preferred_element_type=F32)
            r = r + lax.dot_general(xb[core, :, rows], bb[core, :, cols], DIMS, preferred_element_type=F32)
            r = r + more[row : row + 512, cols].astype(F32)
            out[:, pl.ds(pl.multiple_of(n * 256, 256), 256)] = r.astype(dtype)

    return pl.pallas_call(
        kernel,
        out_shape=shape(512, 512, dtype=dtype),
        in_specs=[VMEM] * 5,
        out_specs=VMEM,
        compiler_params=pltpu.CompilerParams(vmem_limit_bytes=12 << 20),
        cost_estimate=cost(2 * 512 * 512 * 512, 4 << 20),
        name="kept_half",
    )(*tokens, added)


def backward(bga, bgb, u_a, u_b):
    def kernel(a_ref, b_ref, ua_ref, ub_ref, *outs):
        def write(ref, k, u, cols):
            r = lax.dot_general(ref[0], u, (((1,), (1,)), ((), ())), preferred_element_type=F32).astype(BF16)
            outs[k][:, cols], outs[k + 1][:, cols] = r[:128], r[128:]

        @pl.loop(0, 6)
        def _(n):
            u = ua_ref[pl.ds(pl.multiple_of(n * 256, 256), 256)]
            cols = pl.ds(pl.multiple_of(jnp.where(n < 4, n, n + 2) * 256, 256), 256)
            write(a_ref, 0, u, cols)
            write(b_ref, 2, u, cols)

        @pl.loop(0, 2)
        def _(n):
            u = ub_ref[pl.ds(pl.multiple_of(n * 256, 256), 256)]
            cols = pl.ds(pl.multiple_of(1024 + n * 256, 256), 256)
            write(a_ref, 0, u, cols)
            write(b_ref, 2, u, cols)

    return pl.pallas_call(
        kernel,
        out_shape=[shape(128, 2048)] * 4,
        in_specs=[VMEM] * 4,
        out_specs=[VMEM] * 4,
        compiler_params=pltpu.CompilerParams(vmem_limit_bytes=14 << 20),
        cost_estimate=cost(2 * 512 * 2048 * 1024, 8 << 20),
        name="backward",
    )(bga, bgb, u_a, u_b)


def total(parts):
    def kernel(a, b, c, d, o_ref):
        for j in range(16):
            cols = slice(j * 128, (j + 1) * 128)
            dst = pl.ds(pl.multiple_of(block_of(j, True) * 128, 128), 128)
            r = a[:, cols].astype(F32) + b[:, cols].astype(F32) + c[:, cols].astype(F32) + d[:, cols].astype(F32)
            o_ref[:, dst] = r.astype(BF16)

    return pl.pallas_call(
        kernel,
        out_shape=shape(128, 2048),
        in_specs=[VMEM] * 4,
        out_specs=VMEM,
        cost_estimate=cost(4_000_000, 5 << 19),
        compiler_params=pltpu.CompilerParams(vmem_limit_bytes=8 << 20),
        name="total",
    )(*parts)


def sends(g, core_of_z):
    g1, g2, g3 = g
    two = crossed(g2, 2, core_of_z)
    return crossed(g1, 1, core_of_z), two, crossed(g3, -1, core_of_z)


def slab_sum(g0, arrived):
    def kernel(g, a, b, c, *outs):
        for k, o in enumerate(outs):

            @pl.loop(0, 4)
            def _(n):
                rows = pl.ds(pl.multiple_of(k * 128 + n * 32, 32), 32)
                r = g[rows] + a[rows].astype(F32) + b[rows].astype(F32) + c[rows].astype(F32)
                o[pl.ds(pl.multiple_of(n * 32, 32), 32)] = r.astype(o.dtype)

    return pl.pallas_call(
        kernel,
        out_shape=[shape(128, 512, dtype=F32)] + [shape(128, 512)] * 3,
        in_specs=[VMEM] * 4,
        out_specs=[VMEM] * 4,
        cost_estimate=cost(1_000_000, 3 << 20),
        compiler_params=pltpu.CompilerParams(vmem_limit_bytes=8 << 20),
        name="slab_sum",
    )(g0, *arrived)


def block_sum(g, arrived):
    def kernel(g, a, b, c, whole, rounded):
        r = g[...] + a[...].astype(F32) + b[...].astype(F32) + c[...].astype(F32)
        whole[...], rounded[...] = r, r.astype(BF16)

    return pl.pallas_call(
        kernel,
        out_shape=(shape(128, 512, dtype=F32), shape(128, 512)),
        in_specs=[VMEM] * 4,
        out_specs=(VMEM,) * 2,
        cost_estimate=cost(1_000_000, 1 << 20),
        compiler_params=pltpu.CompilerParams(vmem_limit_bytes=8 << 20),
        name="block_sum",
    )(g, *arrived)


def settle(part, far):
    def kernel(a, b, o):
        o[...] = a[...] + b[...].astype(F32)

    return pl.pallas_call(
        kernel,
        out_shape=shape(128, 512, dtype=F32),
        in_specs=[VMEM] * 2,
        out_specs=VMEM,
        cost_estimate=cost(1_000_000, 1 << 19),
        compiler_params=pltpu.CompilerParams(vmem_limit_bytes=8 << 20),
        name="settle",
    )(part, far)


def finish(mine, mine_far, near, scale):
    def kernel(a, b, c, up, down):
        first = lax.axis_index("core") == 0
        one = (a[...] + b[...].astype(F32)) * scale
        two = c[...] * scale
        up[...] = jnp.where(first, one, two)
        down[...] = jnp.where(first, two, one).T

    return pl.pallas_call(
        kernel,
        out_shape=(shape(128, 512, dtype=F32), shape(512, 128, dtype=F32)),
        in_specs=[VMEM] * 3,
        out_specs=(VMEM,) * 2,
        cost_estimate=cost(1_000_000, 1 << 20),
        compiler_params=pltpu.CompilerParams(vmem_limit_bytes=8 << 20),
        name="finish",
    )(mine, mine_far, near)


def step(inputs, cotangent, up_weight, down_weight):
    scale = 1.0 / math.sqrt(inputs.shape[0] * 256)

    kept, sent = prepare_weights(up_weight, down_weight)
    received = swap(sent, "core")
    x0, c0 = prepare_tokens(inputs, cotangent)
    x3, c1 = along_x(x0, 1), along_x(c0, -1)
    c3, x1 = along_x(c0, 1), along_x(x0, -1)
    w = join(kept, received)
    w3, w2, w1 = sends((w, w, w), 0)
    s0 = stack(w, w1, w2, w3)
    s3, s1 = crossed(s0, 1, 1), crossed(s0, -1, 1)
    h3, h1 = near_halves(s3, s1)
    far = crossed(h3, 1, 1), crossed(h1, -1, 1)
    x2, c2 = along_x(x3, 1), along_x(c1, -1)
    own = (s0, s1, s3)
    theirs = tuple(swap(v, "core") for v in own)
    near = forward_near((x0, x1), (c0, c1), own, theirs)
    theirs = swap(far[0], "core"), swap(far[1], "core")
    xb, bga, bgb, u_b = forward_far(near, (x3, x2), (c3, c2), far, theirs)
    xa, u_a = near[0], near[3]
    tokens = (xa, bga, xb, bgb)

    o2 = swap(to_send(tokens, 2), "core")
    o1 = swap(to_send(tokens, 1), "core")
    o30 = swap(to_send(tokens, 3, 0), "core")
    sums = []
    for h in (0, 1):
        g2 = kept_half(tokens, 2, o2, 0, h)
        g1 = kept_half(tokens, 1, o1, 0, h)
        g3 = kept_half(tokens, 3, o30, 0, h)
        g0 = kept_half(tokens, 0, o30, 512, h, F32)
        arrived = sends((g1, g2, g3), 1)
        block, *others = slab_sum(g0, arrived)
        whole, rounded = block_sum(block, sends(others, 0))
        sums.append((whole, swap(rounded, "rep")))
    near = swap(settle(*sums[0]), "core")
    up_grad, down_grad = finish(*sums[1], near, scale)

    back0, back1, back3, back2 = backward(bga, bgb, u_a, u_b)
    b2, b1, b3 = along_x(back2, 2), along_x(back1, 1), along_x(back3, -1)
    return total((back0, b2, b1, b3)), up_grad, down_grad


def solution(mesh):
    torus = Mesh(mesh.devices.reshape(2, 4, 4, 4, 2), ALL)
    return jax.shard_map(
        step,
        mesh=torus,
        in_specs=(P(ALL, None), P(ALL, None), P(("z", "y"), ("x", "core")), P(("x", "core"), ("z", "y"))),
        out_specs=(P(ALL, None), P(("z", "y"), ("x", "core")), P(("x", "core"), ("z", "y"))),
        check_vma=False,
    )
```
